32 devices in a mesh: tp: 8 (over z, x), dp: 4 (over y, core).
Axes of the slice: x: 2, y: 2, z: 4, core: 2. Of those that a mesh axis runs over, the one named last changes fastest.
Arguments:
- tokens: bfloat16 [64, 4096], P(None, 'dp'), may hold values from -6 to 6
- recurrent_state: float32 [2, 64, 262144], P(None, 'dp', 'tp'), may hold values from -24 to 24
- pre_gain: float32 [2, 4096], P(None, 'dp'), may hold values from 0.1 to 1.9
- w_query: bfloat16 [2, 4096, 2048], P(None, 'dp', 'tp'), may hold values from -0.09375 to 0.09375
- w_key: bfloat16 [2, 4096, 2048], P(None, 'dp', 'tp'), may hold values from -0.09375 to 0.09375
- w_value: bfloat16 [2, 4096, 4096], P(None, 'dp', 'tp'), may hold values from -0.09375 to 0.09375
- w_gate: bfloat16 [2, 4096, 4096], P(None, 'dp', 'tp'), may hold values from -0.09375 to 0.09375
- w_decay: bfloat16 [2, 4096, 2048], P(None, 'dp', 'tp'), may hold values from -1 to 1
- decay_bias: float32 [2, 2048], P(None, 'tp'), may hold values from -5 to 3
- head_gain: float32 [2, 128], replicated, may hold values from 0.1 to 1.9
- w_out: bfloat16 [2, 4096, 4096], P(None, 'tp', 'dp'), may hold values from -0.09375 to 0.09375
- post_gain: float32 [2, 4096], P(None, 'dp'), may hold values from 0.1 to 1.9
Outputs:
- hidden_out: bfloat16 [64, 4096], P(None, 'dp')
- state_out: float32 [2, 64, 262144], P(None, 'dp', 'tp')
The draws below stay inside these ranges and needn't reach their ends.
All inputs are finite; a program needn't handle non-finite values.
Results may differ from the reference program's by a relative error of at most 0.015.
Values may be sent and summed in bfloat16 or wider, within the bound.
A program may use at most 64 MiB of HBM per device.

```python
import jax
import jax.numpy as jnp
from jax import lax

D = 4096
HEADS = 32
KEY = 64
VAL = 128
QK = 2048
VW = 4096
SEQS = 64


def draw_recurrent_state(key, part):
    shape = (2, SEQS, VW * KEY)
    column = jnp.arange(VW * KEY, dtype=jnp.int32) // KEY
    within = (column % VAL).astype(jnp.float32) / (VAL - 1)
    ratio = 6.0
    noise = jnp.clip(jax.random.normal(key, shape, jnp.float32), -4.0, 4.0)
    scale = 0.5 * jnp.exp(jnp.log(ratio) * within)
    return (noise * scale[None, None, :]).astype(jnp.float32)


def levels(key, shape, split, smallest, high):
    level = 1.0
    for axis_at, blocks in split:
        heights = jax.random.uniform(jax.random.fold_in(jax.random.fold_in(key, 6), axis_at), (blocks,), jnp.float32, smallest / len(split), high / len(split))
        level = level * jnp.repeat(jnp.exp(heights), shape[axis_at] // blocks).reshape((-1,) + (1,) * (len(shape) - 1 - axis_at))
    return level


def scatter_about(key, shape, scale, reach, cuts=(), kind=jnp.bfloat16):
    values = jax.random.normal(key, shape, jnp.float32) * scale
    if len(cuts) > 0:
        values = levels(key, shape, cuts, -0.22, 0.18) * values
    return jnp.clip(values, min=-reach, max=reach).astype(kind)


def setup_inputs(seed: int = 0) -> dict:
    key_of = jax.random.split(jax.random.key(seed), 13)
    return {
        "tokens": scatter_about(key_of[0], (SEQS, D), 1.0, 6.0, ((1, 4),)),
        "recurrent_state": draw_recurrent_state(jax.random.fold_in(key_of[12], 71), 0),
        "pre_gain": jnp.clip(1.0 + 0.18 * jax.random.normal(key_of[2], (2, D), jnp.float32), 0.1, 1.9),
        "w_query": scatter_about(key_of[3], (2, D, QK), D ** -0.5, 0.09375, ((1, 4), (2, 8))),
        "w_key": scatter_about(key_of[4], (2, D, QK), D ** -0.5, 0.09375, ((1, 4), (2, 8))),
        "w_value": scatter_about(key_of[5], (2, D, VW), D ** -0.5, 0.09375, ((1, 4), (2, 8))),
        "w_gate": scatter_about(key_of[6], (2, D, VW), D ** -0.5, 0.09375, ((1, 4), (2, 8))),
        "w_decay": scatter_about(key_of[7], (2, D, QK), 0.0625, 1.0, ((1, 4), (2, 8))),
        "decay_bias": jnp.clip(-5.0 + 8.0 * jax.random.uniform(key_of[8], (2, QK), jnp.float32) ** levels(key_of[8], (2, QK), ((1, 8),), -0.2, 0.2), -5.0, 3.0),
        "head_gain": jnp.clip(1.0 + 0.18 * jax.random.normal(key_of[9], (2, VAL), jnp.float32), 0.1, 1.9),
        "w_out": scatter_about(key_of[10], (2, VW, D), VW ** -0.5, 0.09375, ((1, 8), (2, 4))),
        "post_gain": jnp.clip(1.0 + 0.18 * jax.random.normal(key_of[11], (2, D), jnp.float32), 0.1, 1.9),
    }


epsilon = 1e-06

def reference(tokens, recurrent_state, pre_gain, w_query, w_key, w_value, w_gate, w_decay, decay_bias, head_gain, w_out, post_gain):
    residual = tokens
    new_states = []
    for section_index in range(2):
        wide_float = residual.astype(jnp.float32)
        row_scale = lax.rsqrt(lax.optimization_barrier(jnp.mean(wide_float * wide_float, axis=1, keepdims=True)) + epsilon)
        normed = (wide_float * pre_gain[section_index]).astype(jnp.bfloat16)

        def project_role(weights):
            return jnp.dot(normed, weights[section_index], preferred_element_type=jnp.float32) * row_scale
        query = lax.optimization_barrier(project_role(w_query).astype(jnp.bfloat16)).astype(jnp.float32)
        key_vec = lax.optimization_barrier(project_role(w_key).astype(jnp.bfloat16)).astype(jnp.float32)
        values_own = project_role(w_value)
        gate_pre = project_role(w_gate)
        log_decay = jax.nn.log_sigmoid(project_role(w_decay) + decay_bias[section_index]) / 16.0
        seq_count = residual.shape[0]
        query = query.reshape(seq_count, HEADS, 1, KEY)
        key_vec = key_vec.reshape(seq_count, HEADS, 1, KEY)
        decay_rate = jnp.exp(log_decay).reshape(seq_count, HEADS, 1, KEY)
        old_state = recurrent_state[section_index].reshape(seq_count, HEADS, VAL, KEY)
        new_state = decay_rate * old_state + key_vec * values_own.reshape(seq_count, HEADS, VAL, 1)
        readout = lax.optimization_barrier(jnp.sum(query * new_state, axis=3)) * KEY ** (-0.5)
        head_mean = lax.optimization_barrier(jnp.mean(readout * readout, axis=-1, keepdims=True))
        mixed = readout * lax.rsqrt(head_mean + epsilon) * head_gain[section_index] * jax.nn.silu(gate_pre.reshape(seq_count, HEADS, VAL))
        mixed = mixed.reshape(seq_count, HEADS * VAL).astype(jnp.bfloat16)
        out_rows = jnp.dot(mixed, w_out[section_index], preferred_element_type=jnp.float32)
        out_scale = lax.rsqrt(lax.optimization_barrier(jnp.mean(out_rows * out_rows, axis=1, keepdims=True)) + epsilon)
        residual = (wide_float + out_rows * out_scale * post_gain[section_index]).astype(jnp.bfloat16)
        new_states.append(new_state.reshape(seq_count, HEADS * VAL * KEY))
    return (residual, jnp.stack(new_states))
```

```python
import functools

import jax
import jax.numpy as jnp
from jax import lax
from jax.experimental import pallas as pl
from jax.experimental.pallas import tpu as pltpu
from jax.sharding import PartitionSpec as P

KEY = 64
VAL = 128
LANES = 128
epsilon = 1e-06
MESH = pl.DeviceIdType.MESH
F32 = jnp.float32
BF16 = jnp.bfloat16


def pad(width):
    return -(-width // LANES) * LANES


def kernel(
    dp, tp, qk, vw, tile,
    tok, st, pre, wq, wk, wv, wg, wd, bias, hgain, wo, post,
    hid, sto,
    W, WO, S, xf, nrm, part, rbuf, sqa, sqb, psum,
    qd2, dec2, k2, vv, base, sg, mg, obuf, rb, sqo, sqr, xg,
    wsem, wosem, ssem, osem, sA, rA, sQ, rQ, sB, rB, sC, rC, sR, rR, sG, rG,
):
    me_dp = lax.axis_index("dp")
    me_tp = lax.axis_index("tp")
    seqs = tok.shape[0]
    rows = seqs // dp
    orows = seqs // tp
    feats = tok.shape[1] * dp
    heads = vw // VAL
    tiles = W.shape[2] // tile
    q_at, k_at, d_at = 0, pad(qk), 2 * pad(qk)
    v_at = 3 * pad(qk)
    g_at = v_at + vw
    sections = ((wq, q_at, pad(qk)), (wk, k_at, pad(qk)), (wd, d_at, pad(qk)), (wv, v_at, vw), (wg, g_at, vw))

    def dp_peer(k):
        return lax.rem(me_dp + k, dp)

    def tp_peer(k):
        return lax.rem(me_tp + k, tp)

    for k in range(1, dp):
        pl.semaphore_signal(pltpu.get_barrier_semaphore(), inc=1, device_id={"dp": dp_peer(k)}, device_id_type=MESH)
    for k in range(1, tp):
        pl.semaphore_signal(pltpu.get_barrier_semaphore(), inc=1, device_id={"tp": tp_peer(k)}, device_id_type=MESH)

    def weight_copy(b, n):
        ref, at, width = sections[n]
        return pltpu.make_async_copy(ref.at[b], W.at[b, :, pl.ds(at, width)], wsem.at[b, n])

    def state_in(b):
        return pltpu.make_async_copy(st.at[b], S.at[b], ssem.at[b])

    def state_out(b):
        return pltpu.make_async_copy(S.at[b], sto.at[b], osem.at[b])

    def wo_copy(b):
        return pltpu.make_async_copy(wo.at[b], WO.at[b], wosem.at[b])

    for b in range(2):
        for n in range(5):
            weight_copy(b, n).start()
        state_in(b).start()
        wo_copy(b).start()

    xf[...] = tok[...].astype(F32)
    lane = lax.broadcasted_iota(jnp.int32, (LANES, LANES), 1)
    depth = lax.broadcasted_iota(jnp.int32, (LANES, LANES), 0)
    reducer = (depth // KEY == lane % 2).astype(F32).astype(BF16)
    lane_row = lax.broadcasted_iota(jnp.int32, (rows, LANES), 1)
    pair_of = lane_row // 2
    low_half = lane_row < KEY
    pairs = VAL // 2

    pl.semaphore_wait(pltpu.get_barrier_semaphore(), dp - 1 + tp - 1)

    def remote(src, dst, send, recv, axis, peer):
        return pltpu.make_async_remote_copy(
            src_ref=src, dst_ref=dst, send_sem=send, recv_sem=recv,
            device_id={axis: peer}, device_id_type=MESH,
        )

    def copy_A(b, t, k):
        return remote(part.at[b, t, dp_peer(k)], rbuf.at[b, t, k], sA.at[b, t, k], rA.at[b, t, k], "dp", dp_peer(k))

    def copy_Q(b, k):
        return remote(sqa.at[b, dp_peer(k)], sqb.at[b, k], sQ.at[b, k], rQ.at[b, k], "dp", dp_peer(k))

    def copy_B(b, k):
        return remote(mg.at[b, me_dp], mg.at[b, me_dp], sB.at[b, k], rB.at[b, k], "dp", dp_peer(k))

    def wait_B(b, k):
        src = lax.rem(me_dp + dp - k, dp)
        remote(mg.at[b, src], mg.at[b, src], sB.at[b, k], rB.at[b, k], "dp", dp_peer(k)).wait_recv()

    def copy_C(b, k):
        return remote(obuf.at[b, tp_peer(k)], rb.at[b, k], sC.at[b, k], rC.at[b, k], "tp", tp_peer(k))

    def copy_R(b, k):
        return remote(sqo.at[b], sqr.at[b, k], sR.at[b, k], rR.at[b, k], "dp", dp_peer(k))

    def copy_G(b, k):
        return remote(xg.at[b, me_tp], xg.at[b, me_tp], sG.at[b, k], rG.at[b, k], "tp", tp_peer(k))

    def wait_G(b, k):
        src = lax.rem(me_tp + tp - k, tp)
        remote(xg.at[b, src], xg.at[b, src], sG.at[b, k], rG.at[b, k], "tp", tp_peer(k)).wait_recv()

    def block(b, carry):
        x = xf[...]
        squares = jnp.sum(x * x, axis=1, keepdims=True)
        sqa[b] = jnp.broadcast_to(squares, (seqs, LANES)).reshape(dp, rows, LANES)
        nrm[...] = (x * pre[pl.ds(b, 1), :]).astype(BF16)
        for k in range(1, dp):
            copy_Q(b, k).start()
        for n in range(5):
            weight_copy(b, n).wait()

        def project(t, c):
            cols = pl.ds(pl.multiple_of(t * tile, tile), tile)
            y = jnp.dot(nrm[...], W[b, :, cols], preferred_element_type=F32)
            part[b, t] = y.reshape(dp, rows, tile).astype(BF16)
            for k in range(1, dp):
                copy_A(b, t, k).start()
            return c

        lax.fori_loop(0, tiles, project, 0)

        total_sq = sqa[b, me_dp]
        for k in range(1, dp):
            copy_Q(b, k).wait_recv()
            total_sq = total_sq + sqb[b, k]
        row_scale = lax.rsqrt(total_sq[:, :1] / feats + epsilon)

        def collect(t, c):
            total = part[b, t, me_dp].astype(F32)
            for k in range(1, dp):
                copy_A(b, t, k).wait_recv()
                total = total + rbuf[b, t, k].astype(F32)
            psum[t] = total * row_scale
            return c

        lax.fori_loop(0, tiles, collect, 0)

        def piece(at, width):
            return psum[at // tile, :, pl.ds(at % tile, width)]

        bias_row = bias[pl.ds(b, 1), :]
        for h in range(heads):
            query = piece(q_at + h * KEY, KEY).astype(BF16).astype(F32)
            key_vec = piece(k_at + h * KEY, KEY).astype(BF16).astype(F32)
            z = piece(d_at + h * KEY, KEY) + bias_row[:, h * KEY : (h + 1) * KEY]
            log_sig = jnp.minimum(z, 0.0) - jnp.log(1.0 + jnp.exp(-jnp.abs(z)))
            decay = jnp.exp(log_sig / 16.0)
            value = piece(v_at + h * VAL, VAL)
            gate = piece(g_at + h * VAL, VAL)
            qd = query * decay
            qd2[h] = jnp.concatenate([qd, qd], axis=1)
            dec2[h] = jnp.concatenate([decay, decay], axis=1)
            k2[h] = jnp.concatenate([key_vec, key_vec], axis=1)
            vv[h] = value
            base[h] = jnp.sum(query * key_vec, axis=1, keepdims=True) * value
            sg[h] = gate / (1.0 + jnp.exp(-gate))

        state_in(b).wait()

        def readout(h, c):
            at = pl.multiple_of(h * VAL * KEY, LANES)
            qd = qd2[h]
            prods = jnp.concatenate(
                [S[b, :, pl.ds(at + j * LANES, LANES)] * qd for j in range(pairs)], axis=0
            ).astype(BF16)
            sums = jnp.dot(prods, reducer, preferred_element_type=F32)
            acc = base[h]
            for j in range(pairs):
                acc = acc + jnp.where(pair_of == j, sums[j * rows : (j + 1) * rows], 0.0)
            read = acc * KEY ** (-0.5)
            mean = jnp.mean(read * read, axis=1, keepdims=True)
            mixed = read * lax.rsqrt(mean + epsilon) * hgain[pl.ds(b, 1), :] * sg[h]
            mg[b, me_dp, :, pl.ds(pl.multiple_of(h * VAL, VAL), VAL)] = mixed.astype(BF16)
            return c

        lax.fori_loop(0, heads, readout, 0)
        for k in range(1, dp):
            copy_B(b, k).start()
        wo_copy(b).wait()
        for k in range(1, dp):
            wait_B(b, k)
        out = jnp.dot(mg[b].reshape(seqs, vw), WO[b], preferred_element_type=F32)
        obuf[b] = out.reshape(tp, orows, out.shape[1]).astype(BF16)
        for k in range(1, tp):
            copy_C(b, k).start()

        def update(h, c):
            at = pl.multiple_of(h * VAL * KEY, LANES)
            decay, key_vec, value = dec2[h], k2[h], vv[h]
            for j in range(pairs):
                here = pl.ds(at + j * LANES, LANES)
                spread = jnp.where(low_half, value[:, 2 * j : 2 * j + 1], value[:, 2 * j + 1 : 2 * j + 2])
                S[b, :, here] = decay * S[b, :, here] + key_vec * spread
            return c

        lax.fori_loop(0, heads, update, 0)
        state_out(b).start()

        total = obuf[b, me_tp].astype(F32)
        for k in range(1, tp):
            copy_C(b, k).wait_recv()
            total = total + rb[b, k].astype(F32)
        own_sq = jnp.broadcast_to(jnp.sum(total * total, axis=1, keepdims=True), (orows, LANES))
        sqo[b] = own_sq
        for k in range(1, dp):
            copy_R(b, k).start()
        mine = xf[pl.ds(pl.multiple_of(me_tp * orows, orows), orows), :]
        gained = total * post[pl.ds(b, 1), :]
        for k in range(1, dp):
            copy_R(b, k).wait_recv()
            own_sq = own_sq + sqr[b, k]
        out_scale = lax.rsqrt(own_sq[:, :1] / feats + epsilon)
        xg[b, me_tp] = (mine + gained * out_scale).astype(BF16)
        for k in range(1, tp):
            copy_G(b, k).start()
        for k in range(1, tp):
            wait_G(b, k)
        xf[...] = xg[b].astype(F32).reshape(seqs, xf.shape[1])

        for k in range(1, dp):
            copy_Q(b, k).wait_send()
            copy_B(b, k).wait_send()
            copy_R(b, k).wait_send()

        def drain(t, c):
            for k in range(1, dp):
                copy_A(b, t, k).wait_send()
            return c

        lax.fori_loop(0, tiles, drain, 0)
        for k in range(1, tp):
            copy_C(b, k).wait_send()
            copy_G(b, k).wait_send()
        return carry

    lax.fori_loop(0, 2, block, 0)
    hid[...] = xf[...].astype(BF16)
    for b in range(2):
        state_out(b).wait()


def solution(mesh):
    dp, tp = mesh.shape["dp"], mesh.shape["tp"]

    def local(tok, st, pre, wq, wk, wv, wg, wd, bias, hgain, wo, post):
        seqs, width = tok.shape
        rows, orows = seqs // dp, seqs // tp
        qk, vw = wq.shape[2], wv.shape[2]
        if pad(qk) != qk:
            fill = ((0, 0), (0, 0), (0, pad(qk) - qk))
            wq, wk, wd = (jnp.pad(w, fill) for w in (wq, wk, wd))
        heads = vw // VAL
        total = 3 * pad(qk) + 2 * vw
        tile = 2 * LANES if total % (2 * LANES) == 0 and pad(qk) % (2 * LANES) == 0 else LANES
        tiles = total // tile
        vmem = pl.BlockSpec(memory_space=pltpu.VMEM)
        hbm = pl.BlockSpec(memory_space=pl.ANY)
        dma = pltpu.SemaphoreType.DMA
        per_head = pltpu.VMEM((heads, rows, LANES), F32)
        return pl.pallas_call(
            functools.partial(kernel, dp, tp, qk, vw, tile),
            out_shape=(
                jax.ShapeDtypeStruct(tok.shape, BF16),
                jax.ShapeDtypeStruct(st.shape, F32),
            ),
            in_specs=[vmem, hbm, vmem, hbm, hbm, hbm, hbm, hbm, vmem, vmem, hbm, vmem],
            out_specs=(vmem, hbm),
            scratch_shapes=[
                pltpu.VMEM((2, width, total), BF16),
                pltpu.VMEM((2,) + wo.shape[1:], BF16),
                pltpu.VMEM(st.shape, F32),
                pltpu.VMEM((seqs, width), F32),
                pltpu.VMEM((seqs, width), BF16),
                pltpu.VMEM((2, tiles, dp, rows, tile), BF16),
                pltpu.VMEM((2, tiles, dp, rows, tile), BF16),
                pltpu.VMEM((2, dp, rows, LANES), F32),
                pltpu.VMEM((2, dp, rows, LANES), F32),
                pltpu.VMEM((tiles, rows, tile), F32),
                per_head, per_head, per_head, per_head, per_head, per_head,
                pltpu.VMEM((2, dp, rows, vw), BF16),
                pltpu.VMEM((2, tp, orows, width), BF16),
                pltpu.VMEM((2, tp, orows, width), BF16),
                pltpu.VMEM((2, orows, LANES), F32),
                pltpu.VMEM((2, dp, orows, LANES), F32),
                pltpu.VMEM((2, tp, orows, width), BF16),
                dma((2, 5)), dma((2,)), dma((2,)), dma((2,)),
                dma((2, tiles, dp)), dma((2, tiles, dp)),
                dma((2, dp)), dma((2, dp)),
                dma((2, dp)), dma((2, dp)),
                dma((2, tp)), dma((2, tp)),
                dma((2, dp)), dma((2, dp)),
                dma((2, tp)), dma((2, tp)),
            ],
            compiler_params=pltpu.CompilerParams(
                collective_id=0, has_side_effects=True, vmem_limit_bytes=60 * 2**20
            ),
        )(tok, st, pre, wq, wk, wv, wg, wd, bias, hgain, wo, post)

    in_specs = (
        P(None, "dp"),
        P(None, "dp", "tp"),
        P(None, "dp"),
        P(None, "dp", "tp"),
        P(None, "dp", "tp"),
        P(None, "dp", "tp"),
        P(None, "dp", "tp"),
        P(None, "dp", "tp"),
        P(None, "tp"),
        P(),
        P(None, "tp", "dp"),
        P(None, "dp"),
    )
    out_specs = (P(None, "dp"), P(None, "dp", "tp"))
    return jax.shard_map(local, mesh=mesh, in_specs=in_specs, out_specs=out_specs, check_vma=False)
```

```python
import functools

import jax
import jax.numpy as jnp
from jax import lax
from jax.experimental import pallas as pl
from jax.experimental.pallas import tpu as pltpu
from jax.sharding import PartitionSpec as P

KEY = 64
VAL = 128
LANES = 128
epsilon = 1e-06
MESH = pl.DeviceIdType.MESH
F32 = jnp.float32
BF16 = jnp.bfloat16


def pad(width):
    return -(-width // LANES) * LANES


def kernel(
    dp, tp, qk, vw, tile,
    st, wq, wk, wv, wg, wd, wo, tok_in, pre_in, bias_in, hgain_in, post_in,
    hid, S,
    tok, pre, bias, hgain, post, W, WO, xf, nrm, part, rbuf, sqa, sqb, psum,
    qd2, dec2, k2, vv, base, sg, mg, obuf, rb, sqr, xg,
    small, wsem, wosem, ssem, sA, rA, sQ, rQ, sB, rB, sC, rC, sR, rR, sG, rG,
):
    me_dp = lax.axis_index("dp")
    me_tp = lax.axis_index("tp")
    seqs = tok.shape[0]
    rows = seqs // dp
    orows = seqs // tp
    feats = tok.shape[1] * dp
    heads = vw // VAL
    tiles = W.shape[2] // tile
    q_at, k_at, d_at = 0, pad(qk), 2 * pad(qk)
    v_at = 3 * pad(qk)
    g_at = v_at + vw
    sections = ((wq, q_at, pad(qk)), (wk, k_at, pad(qk)), (wd, d_at, pad(qk)), (wv, v_at, vw), (wg, g_at, vw))

    def dp_peer(k):
        return lax.rem(me_dp + k, dp)

    def tp_peer(k):
        return lax.rem(me_tp + k, tp)

    every = dp * tp
    me = me_tp * dp + me_dp

    small_copies = [
        pltpu.make_async_copy(src, dst, small.at[n])
        for n, (src, dst) in enumerate(
            ((tok_in, tok), (pre_in, pre), (bias_in, bias), (hgain_in, hgain), (post_in, post))
        )
    ]
    dp_peers = [me_dp] + [dp_peer(k) for k in range(1, dp)]

    def visit(act):
        def step(kt, c):
            target = tp_peer(kt)
            for kd in range(dp):
                act(kt, kd, {"tp": target, "dp": dp_peers[kd]})
            return c

        for kd in range(1, dp):
            act(0, kd, {"dp": dp_peers[kd]})
        lax.fori_loop(1, tp, step, 0)

    def greet(kt, kd, target):
        pl.semaphore_signal(pltpu.get_barrier_semaphore(), inc=1, device_id=target, device_id_type=MESH)

    def weight_copy(b, n):
        ref, at, width = sections[n]
        return pltpu.make_async_copy(ref.at[b], W.at[b, :, pl.ds(at, width)], wsem.at[b, n])

    def state_in(b):
        return pltpu.make_async_copy(st.at[b], S.at[b], ssem.at[b])

    def wo_copy(b):
        return pltpu.make_async_copy(wo.at[b], WO.at[b], wosem.at[b])

    for copy in small_copies:
        copy.start()
    for n in range(5):
        weight_copy(0, n).start()
    visit(greet)
    lane = lax.broadcasted_iota(jnp.int32, (LANES, LANES), 1)
    depth = lax.broadcasted_iota(jnp.int32, (LANES, LANES), 0)
    reducer = (depth // KEY == lane % 2).astype(F32).astype(BF16)
    lane_row = lax.broadcasted_iota(jnp.int32, (rows, LANES), 1)
    pair_of = lane_row // 2
    low_half = lane_row < KEY
    pairs = VAL // 2
    diagonal = lax.broadcasted_iota(jnp.int32, (orows, LANES), 0) == lax.broadcasted_iota(jnp.int32, (orows, LANES), 1)

    def remote(src, dst, send, recv, axis, peer):
        return pltpu.make_async_remote_copy(
            src_ref=src, dst_ref=dst, send_sem=send, recv_sem=recv,
            device_id={axis: peer}, device_id_type=MESH,
        )

    def copy_A(b, t, k):
        return remote(part.at[b, t, dp_peer(k)], rbuf.at[b, t, k], sA.at[b, t, k], rA.at[b, t, k], "dp", dp_peer(k))

    def copy_Q(b, k):
        return remote(sqa.at[b, dp_peer(k)], sqb.at[b, k], sQ.at[b, k], rQ.at[b, k], "dp", dp_peer(k))

    def copy_B(b, h, k):
        own = mg.at[b, me_dp, h]
        return remote(own, own, sB.at[b, h, k], rB.at[b, h, k], "dp", dp_peer(k))

    def wait_B(b, h, k):
        src = mg.at[b, lax.rem(me_dp + dp - k, dp), h]
        remote(src, src, sB.at[b, h, k], rB.at[b, h, k], "dp", dp_peer(k)).wait_recv()

    def copy_C(b, k):
        return remote(obuf.at[b, tp_peer(k)], rb.at[b, k], sC.at[b, k], rC.at[b, k], "tp", tp_peer(k))

    def send_R(b, kt, kd, target):
        pltpu.make_async_remote_copy(
            src_ref=sqr.at[b, 0], dst_ref=sqr.at[b, kt * dp + kd], send_sem=sR.at[b], recv_sem=rR.at[b],
            device_id=target, device_id_type=MESH,
        ).start()

    def all_R(b):
        others = sqr.at[b, pl.ds(1, every - 1)]
        return remote(others, others, sR.at[b], rR.at[b], "dp", dp_peer(1))

    def copy_G(b, k):
        return remote(xg.at[b, me_tp], xg.at[b, me_tp], sG.at[b, k], rG.at[b, k], "tp", tp_peer(k))

    def wait_G(b, k):
        src = lax.rem(me_tp + tp - k, tp)
        remote(xg.at[b, src], xg.at[b, src], sG.at[b, k], rG.at[b, k], "tp", tp_peer(k)).wait_recv()

    first_tile = [at // tile for _, at, _ in sections]

    def send_tile(b, t):
        for k in range(1, dp):
            copy_A(b, t, k).start()

    def project(b, send):
        x = xf[...]
        squares = jnp.sum(x * x, axis=1, keepdims=True)
        sqa[b] = jnp.broadcast_to(squares, (seqs, LANES)).reshape(dp, rows, LANES)
        nrm[...] = (x * pre[pl.ds(b, 1), :]).astype(BF16)
        if send:
            for k in range(1, dp):
                copy_Q(b, k).start()
        for t in range(tiles):
            if t in first_tile:
                weight_copy(b, first_tile.index(t)).wait()
            y = jnp.dot(nrm[...], W[b, :, t * tile : (t + 1) * tile], preferred_element_type=F32)
            part[b, t] = y.reshape(dp, rows, tile).astype(BF16)
            if send:
                send_tile(b, t)

    for copy in small_copies:
        copy.wait()
    xf[...] = tok[...].astype(F32)
    project(0, False)
    state_in(0).start()
    wo_copy(0).start()
    for n in range(5):
        weight_copy(1, n).start()
    state_in(1).start()
    wo_copy(1).start()
    pl.semaphore_wait(pltpu.get_barrier_semaphore(), every - 1)
    for k in range(1, dp):
        copy_Q(0, k).start()
    for t in range(tiles):
        send_tile(0, t)

    def block(b, carry):
        total_sq = sqa[b, me_dp]
        for k in range(1, dp):
            copy_Q(b, k).wait_recv()
            total_sq = total_sq + sqb[b, k]
        row_scale = lax.rsqrt(total_sq[:, :1] / feats + epsilon)

        def collect(t, c):
            total = part[b, t, me_dp].astype(F32)
            for k in range(1, dp):
                copy_A(b, t, k).wait_recv()
                total = total + rbuf[b, t, k].astype(F32)
            psum[t] = total * row_scale
            return c

        lax.fori_loop(0, tiles, collect, 0)

        def piece(at, width):
            return psum[at // tile, :, pl.ds(at % tile, width)]

        bias_row = bias[pl.ds(b, 1), :]
        for h in range(heads):
            query = piece(q_at + h * KEY, KEY).astype(BF16).astype(F32)
            key_vec = piece(k_at + h * KEY, KEY).astype(BF16).astype(F32)
            z = piece(d_at + h * KEY, KEY) + bias_row[:, h * KEY : (h + 1) * KEY]
            log_sig = jnp.minimum(z, 0.0) - jnp.log(1.0 + jnp.exp(-jnp.abs(z)))
            decay = jnp.exp(log_sig / 16.0)
            value = piece(v_at + h * VAL, VAL)
            gate = piece(g_at + h * VAL, VAL)
            qd = query * decay
            qd2[h] = jnp.concatenate([qd, qd], axis=1)
            dec2[h] = jnp.concatenate([decay, decay], axis=1)
            k2[h] = jnp.concatenate([key_vec, key_vec], axis=1)
            vv[h] = value
            base[h] = jnp.sum(query * key_vec, axis=1, keepdims=True) * value
            sg[h] = gate / (1.0 + jnp.exp(-gate))

        state_in(b).wait()

        def readout(h, c):
            at = pl.multiple_of(h * VAL * KEY, LANES)
            qd = qd2[h]
            prods = jnp.concatenate(
                [S[b, :, pl.ds(at + j * LANES, LANES)] * qd for j in range(pairs)], axis=0
            ).astype(BF16)
            sums = jnp.dot(prods, reducer, preferred_element_type=F32)
            acc = base[h]
            for j in range(pairs):
                acc = acc + jnp.where(pair_of == j, sums[j * rows : (j + 1) * rows], 0.0)
            read = acc * KEY ** (-0.5)
            mean = jnp.mean(read * read, axis=1, keepdims=True)
            mixed = read * lax.rsqrt(mean + epsilon) * hgain[pl.ds(b, 1), :] * sg[h]
            mg[b, me_dp, h] = mixed.astype(BF16)
            for k in range(1, dp):
                copy_B(b, h, k).start()
            return c

        lax.fori_loop(0, heads, readout, 0)
        wo_copy(b).wait()
        for h in range(heads):
            for k in range(1, dp):
                wait_B(b, h, k)
        mixed_all = jnp.concatenate([mg[b, :, h].reshape(seqs, VAL) for h in range(heads)], axis=1)
        out = jnp.dot(mixed_all, WO[b], preferred_element_type=F32)
        obuf[b] = out.reshape(tp, orows, out.shape[1]).astype(BF16)
        for k in range(1, tp):
            copy_C(b, k).start()

        def update(h, c):
            at = pl.multiple_of(h * VAL * KEY, LANES)
            decay, key_vec, value = dec2[h], k2[h], vv[h]
            for j in range(pairs):
                here = pl.ds(at + j * LANES, LANES)
                spread = jnp.where(low_half, value[:, 2 * j : 2 * j + 1], value[:, 2 * j + 1 : 2 * j + 2])
                S[b, :, here] = decay * S[b, :, here] + key_vec * spread
            return c

        lax.fori_loop(0, heads, update, 0)

        total = obuf[b, me_tp].astype(F32)
        for k in range(1, tp):
            copy_C(b, k).wait_recv()
            total = total + rb[b, k].astype(F32)
        own_sq = jnp.broadcast_to(jnp.sum(total * total, axis=1, keepdims=True), (orows, LANES))
        sqr[b, 0] = jnp.sum(jnp.where(diagonal, own_sq, 0.0), axis=0, keepdims=True)
        xg[b, me_tp] = total.astype(BF16)

        for k in range(tp - 1, 0, -1):
            copy_G(b, k).start()
        visit(functools.partial(send_R, b))
        all_R(b).wait_recv()
        for k in range(1, tp):
            wait_G(b, k)

        for t in range(tp):
            from_tp = lax.rem(me_tp + tp - t, tp) * dp
            out_sq = jnp.zeros((1, LANES), F32)
            for d in range(dp):
                out_sq = out_sq + sqr[b, from_tp + lax.rem(me_dp + dp - d, dp)]
            spread = jnp.where(diagonal, jnp.broadcast_to(out_sq, (orows, LANES)), 0.0)
            out_scale = lax.rsqrt(jnp.sum(spread, axis=1, keepdims=True) / feats + epsilon)
            here = pl.ds(t * orows, orows)
            fresh = xf[here, :] + xg[b, t].astype(F32) * out_scale * post[pl.ds(b, 1), :]
            xf[here, :] = fresh.astype(BF16).astype(F32)

        @pl.when(b == 0)
        def _():
            project(1, True)

        for k in range(1, dp):
            copy_Q(b, k).wait_send()
            for h in range(heads):
                copy_B(b, h, k).wait_send()
        all_R(b).wait_send()

        def drain(t, c):
            for k in range(1, dp):
                copy_A(b, t, k).wait_send()
            return c

        lax.fori_loop(0, tiles, drain, 0)
        for k in range(1, tp):
            copy_C(b, k).wait_send()
            copy_G(b, k).wait_send()
        return carry

    lax.fori_loop(0, 2, block, 0)
    hid[...] = xf[...].astype(BF16)


def store_kernel(hid, st, hid_out, st_out, sems):
    copies = [pltpu.make_async_copy(hid, hid_out, sems.at[0])]
    for b in range(2):
        copies.append(pltpu.make_async_copy(st.at[b], st_out.at[b], sems.at[1 + b]))
    for copy in copies:
        copy.start()
    for copy in copies:
        copy.wait()


def solution(mesh):
    dp, tp = mesh.shape["dp"], mesh.shape["tp"]

    def local(tok, st, pre, wq, wk, wv, wg, wd, bias, hgain, wo, post):
        seqs, width = tok.shape
        rows, orows = seqs // dp, seqs // tp
        qk, vw = wq.shape[2], wv.shape[2]
        if pad(qk) != qk:
            fill = ((0, 0), (0, 0), (0, pad(qk) - qk))
            wq, wk, wd = (jnp.pad(w, fill) for w in (wq, wk, wd))
        heads = vw // VAL
        total = 3 * pad(qk) + 2 * vw
        tile = 2 * LANES if total % (2 * LANES) == 0 and pad(qk) % (2 * LANES) == 0 else LANES
        tiles = total // tile
        arrays = tuple(
            pltpu.with_memory_space_constraint(array, pltpu.HBM)
            for array in (st, wq, wk, wv, wg, wd, wo, tok, pre, bias, hgain, post)
        )
        vmem = pl.BlockSpec(memory_space=pltpu.VMEM)
        hbm = pl.BlockSpec(memory_space=pl.ANY)
        dma = pltpu.SemaphoreType.DMA
        per_head = pltpu.VMEM((heads, rows, LANES), F32)
        hid, new_state = pl.pallas_call(
            functools.partial(kernel, dp, tp, qk, vw, tile),
            out_shape=(pltpu.VMEM(tok.shape, BF16), pltpu.VMEM(st.shape, F32)),
            in_specs=[hbm] * 12,
            out_specs=(vmem, vmem),
            scratch_shapes=[
                *(pltpu.VMEM(a.shape, a.dtype) for a in (tok, pre, bias, hgain, post)),
                pltpu.VMEM((2, width, total), BF16),
                pltpu.VMEM((2,) + wo.shape[1:], BF16),
                pltpu.VMEM((seqs, width), F32),
                pltpu.VMEM((seqs, width), BF16),
                pltpu.VMEM((2, tiles, dp, rows, tile), BF16),
                pltpu.VMEM((2, tiles, dp, rows, tile), BF16),
                pltpu.VMEM((2, dp, rows, LANES), F32),
                pltpu.VMEM((2, dp, rows, LANES), F32),
                pltpu.VMEM((tiles, rows, tile), F32),
                per_head, per_head, per_head, per_head, per_head, per_head,
                pltpu.VMEM((2, dp, heads, rows, VAL), BF16),
                pltpu.VMEM((2, tp, orows, width), BF16),
                pltpu.VMEM((2, tp, orows, width), BF16),
                pltpu.VMEM((2, dp * tp, 1, LANES), F32),
                pltpu.VMEM((2, tp, orows, width), BF16),
                dma((5,)), dma((2, 5)), dma((2,)), dma((2,)),
                dma((2, tiles, dp)), dma((2, tiles, dp)),
                dma((2, dp)), dma((2, dp)),
                dma((2, heads, dp)), dma((2, heads, dp)),
                dma((2, tp)), dma((2, tp)),
                dma((2,)), dma((2,)),
                dma((2, tp)), dma((2, tp)),
            ],
            compiler_params=pltpu.CompilerParams(
                collective_id=0, has_side_effects=True, vmem_limit_bytes=24 * 2**20
            ),
        )(*arrays)
        return pl.pallas_call(
            store_kernel,
            out_shape=(
                jax.ShapeDtypeStruct(tok.shape, BF16),
                jax.ShapeDtypeStruct(st.shape, F32),
            ),
            in_specs=[hbm, hbm],
            out_specs=(hbm, hbm),
            scratch_shapes=[dma((3,))], compiler_params=pltpu.CompilerParams(vmem_limit_bytes=2**20),
        )(pltpu.with_memory_space_constraint(hid, pltpu.VMEM), pltpu.with_memory_space_constraint(new_state, pltpu.VMEM))

    in_specs = (
        P(None, "dp"),
        P(None, "dp", "tp"),
        P(None, "dp"),
        P(None, "dp", "tp"),
        P(None, "dp", "tp"),
        P(None, "dp", "tp"),
        P(None, "dp", "tp"),
        P(None, "dp", "tp"),
        P(None, "tp"),
        P(),
        P(None, "tp", "dp"),
        P(None, "dp"),
    )
    out_specs = (P(None, "dp"), P(None, "dp", "tp"))
    return jax.shard_map(local, mesh=mesh, in_specs=in_specs, out_specs=out_specs, check_vma=False)
```
